32 devices in a mesh: ep: 8 (over z, y), tp: 4 (over x, core).
Axes of the slice: x: 2, y: 2, z: 4, core: 2. Of those that a mesh axis runs over, the one named last changes fastest.
Arguments:
- tokens: bfloat16 [1024, 2048], P('ep', 'tp'), may hold values from -6 to 6
- norm_gain: bfloat16 [2048], P('tp'), may hold values from 0.099609375 to 1.8984375
- routes: int32 [1024, 2], P('ep'), may hold values from 0 to 7, as said below
- gate_weights: float32 [1024, 2], P('ep'), may hold values from 0.1 to 1
- w_gate: bfloat16 [8, 2048, 4096], P('ep', None, 'tp'), may hold values from -0.125 to 0.125
- w_up: bfloat16 [8, 2048, 4096], P('ep', None, 'tp'), may hold values from -0.125 to 0.125
- w_down: bfloat16 [8, 4096, 2048], P('ep', 'tp'), may hold values from -0.875 to 0.875
- out_gain: bfloat16 [2048], P('tp'), may hold values from 0.099609375 to 1.8984375
Outputs:
- mixed: bfloat16 [1024, 2048], P('ep', 'tp')
The draws below stay inside these ranges and needn't reach their ends.
Inputs may be any that keep to these rules, and one draw needn't show every extreme that they name: `routes`: each row names 2 different experts of one group (their quotients by 8 agree). In each aligned block of 128 rows no expert is named by more than 64 rows, and in every block some expert is named by exactly 64 rows.
All inputs are finite; a program needn't handle non-finite values.
Results may differ from the reference program's by a relative error of at most 0.019.
Values may be sent and summed in bfloat16 or wider, within the bound.
A program may use at most 64 MiB of HBM per device.

```python
import math
import jax
import jax.numpy as jnp
from jax import lax

D = 2048
FF = 4096
EPG = 8
TOPK = 2
TOK_DEV = 128
EXPERTS = 8
GROUPS = 1
MEAN = 32
CAP = 64
TOKENS = 1024
N_EP = 8
N_TP = 4


def draw_routes(key, part):
    folded = jax.random.fold_in(key, 5)
    k_pop, k_jit, k_perm = jax.random.split(folded, 3)
    popular = jax.random.randint(k_pop, (EXPERTS,), 0, 4)
    jitter = jax.random.randint(k_jit, (N_EP, EXPERTS), 0, 3)
    expert_ids = jnp.arange(EXPERTS, dtype=jnp.int32)
    scores = (popular[None, :] * 4 + jitter) * EXPERTS + expert_ids[None, :]
    sorted_ids = jnp.argsort(scores, axis=1)
    ranking = jnp.argsort(sorted_ids, axis=1)
    quarter = ranking * 4 // EXPERTS
    counts = jnp.where(quarter == 3, 2 * MEAN, jnp.where(quarter == 2, MEAN, MEAN // 2)).astype(jnp.int32)
    group_copies = counts.reshape(N_EP, GROUPS, EPG).sum(axis=2)
    group_tokens = group_copies // 2
    token_end = jnp.cumsum(group_tokens, axis=1)
    token_start = token_end - group_tokens
    copy_start = jnp.cumsum(group_copies, axis=1) - group_copies
    expert_end = jnp.cumsum(counts, axis=1)
    positions = jnp.arange(TOK_DEV, dtype=jnp.int32)
    group_of = jnp.sum(positions[None, :, None] >= token_end[:, None, :], axis=2).astype(jnp.int32)
    within = positions[None, :] - jnp.take_along_axis(token_start, group_of, axis=1)
    first_copy = jnp.take_along_axis(copy_start, group_of, axis=1) + within
    second_copy = first_copy + jnp.take_along_axis(group_tokens, group_of, axis=1)

    def owner_of(copies):
        return jnp.sum(copies[:, :, None] >= expert_end[:, None, :], axis=2).astype(jnp.int32)
    chosen = jnp.stack([owner_of(first_copy), owner_of(second_copy)], axis=2)
    shuffle = jax.random.randint(k_perm, (N_EP, TOK_DEV), 0, 1 << 20) * TOK_DEV + positions[None, :]
    shuffled_order = jnp.argsort(shuffle, axis=1)
    chosen = jnp.take_along_axis(chosen, shuffled_order[:, :, None], axis=1)
    return chosen.reshape(N_EP * TOK_DEV, 2).astype(jnp.int32)


def draw_w_down(key, part):
    k_base, k_rough = jax.random.split(jax.random.fold_in(key, 7))
    column = jnp.arange(D, dtype=jnp.float32) / D
    base = jnp.clip(jax.random.normal(k_base, (EXPERTS, FF, D), jnp.float32), -4.0, 4.0)
    rising = 10.0 ** column
    rough = jax.random.uniform(k_rough, (D,), jnp.float32, 0.6, 1.4)
    return (base * (rising * rough / FF ** 0.5)[None, None, :]).astype(jnp.bfloat16)


def block_levels(own_key, shape, pieces, least, largest):
    def one(axis_at, parts):
        draws = jax.random.uniform(jax.random.fold_in(jax.random.fold_in(own_key, 6), axis_at), (parts,), jnp.float32, least / len(pieces), largest / len(pieces))
        return jnp.repeat(jnp.exp(draws), shape[axis_at] // parts).reshape((-1,) + (1,) * (len(shape) - axis_at - 1))

    gain = one(*pieces[0])
    for cut in pieces[1:]:
        gain = gain * one(*cut)
    return gain


def bell_draw(rng, extent, width, limit, shards=(), held_as=jnp.bfloat16):
    factor_of = block_levels(rng, extent, shards, -0.22, 0.18) if shards else 1.0
    result = jax.random.normal(rng, extent, jnp.float32) * width * factor_of
    return jnp.minimum(jnp.maximum(result, -limit), limit).astype(held_as)


def setup_inputs(seed: int = 0) -> dict:
    keys = jax.random.split(jax.random.key(seed), 9)
    tokens = bell_draw(keys[0], (TOKENS, D), 1.0, 6.0, ((0, 8), (1, 4)))
    norm_gain = jnp.clip(1.0 + 0.18 * jax.random.normal(keys[1], (D,), jnp.float32), 0.099609375, 1.8984375).astype(jnp.bfloat16)
    routes = draw_routes(jax.random.fold_in(keys[8], 71), 0)
    gate_weights = jnp.clip(jnp.exp(math.log(1.0) - 2.3025851 * jax.random.uniform(keys[3], (TOKENS, TOPK), jnp.float32) ** block_levels(keys[3], (TOKENS, TOPK), ((0, 8),), -0.2, 0.2)), 0.1, 1.0)
    w_gate = bell_draw(keys[4], (EXPERTS, D, FF), D ** -0.5, 0.125, ((0, 8), (2, 4)))
    w_up = bell_draw(keys[5], (EXPERTS, D, FF), D ** -0.5, 0.125, ((0, 8), (2, 4)))
    w_down = draw_w_down(jax.random.fold_in(keys[8], 71), 0)
    out_gain = jnp.clip(1.0 + 0.18 * jax.random.normal(keys[7], (D,), jnp.float32), 0.099609375, 1.8984375).astype(jnp.bfloat16)
    return dict(tokens=tokens, norm_gain=norm_gain, routes=routes, gate_weights=gate_weights, w_gate=w_gate, w_up=w_up, w_down=w_down, out_gain=out_gain)


epsilon = 1e-06

def route_slots(routes):
    blocks = routes.reshape(N_EP, TOK_DEV * TOPK)
    onehot = (blocks[:, :, None] == jnp.arange(EXPERTS, dtype=jnp.int32)[None, None, :]).astype(jnp.int32)
    before = jnp.cumsum(onehot, axis=1) - onehot
    return lax.optimization_barrier(jnp.sum(before * onehot, axis=2)).astype(jnp.int32)

def reference(tokens, norm_gain, routes, gate_weights, w_gate, w_up, w_down, out_gain):
    x_float = tokens.astype(jnp.float32)
    scale_in = lax.rsqrt(lax.optimization_barrier(jnp.mean(x_float * x_float, axis=1, keepdims=True)) + epsilon)
    normed = (x_float * scale_in * norm_gain.astype(jnp.float32)).astype(jnp.bfloat16)
    slot_index = route_slots(routes)
    expert_ids = routes.reshape(N_EP, TOK_DEV * TOPK).astype(jnp.int32)
    source = jnp.arange(N_EP, dtype=jnp.int32)[:, None]
    copy_ids = jnp.arange(TOK_DEV * TOPK, dtype=jnp.int32)[None, :]
    token_ids = (source * TOK_DEV + copy_ids // TOPK).astype(jnp.int32)
    buffer_pos = (source * CAP + slot_index).astype(jnp.int32)
    table = jnp.full((EXPERTS, N_EP * CAP), TOKENS, jnp.int32).at[expert_ids, buffer_pos].set(token_ids)
    padded = jnp.concatenate([normed, jnp.zeros((1, D), jnp.bfloat16)], axis=0)

    def expert(inputs):
        row_table, gate_mat, up_mat, down_mat = inputs
        arrived = padded[row_table]
        gate_sum = jnp.dot(arrived, gate_mat, preferred_element_type=jnp.float32)
        up_sum = jnp.dot(arrived, up_mat, preferred_element_type=jnp.float32)
        hidden = (jax.nn.silu(gate_sum) * up_sum).astype(jnp.bfloat16)
        hidden_blocks = hidden.reshape(N_EP * CAP, N_TP, FF // N_TP).astype(jnp.float32)
        down_blocks = down_mat.reshape(N_TP, FF // N_TP, D).astype(jnp.float32)
        partial_value = jnp.einsum('rtf,tfd->trd', hidden_blocks, down_blocks).astype(jnp.bfloat16)
        partial_value = lax.optimization_barrier(partial_value)
        return lax.optimization_barrier(jnp.sum(partial_value.astype(jnp.float32), axis=0)).astype(jnp.bfloat16)
    outputs = lax.map(expert, (table, w_gate, w_up, w_down))
    picked = outputs[expert_ids, buffer_pos].astype(jnp.float32).reshape(TOKENS, TOPK, D)
    combined = lax.optimization_barrier(jnp.sum(picked * gate_weights[:, :, None], axis=1))
    scale_out = lax.rsqrt(lax.optimization_barrier(jnp.mean(combined * combined, axis=1, keepdims=True)) + epsilon)
    return (combined * scale_out * out_gain.astype(jnp.float32)).astype(jnp.bfloat16)
```

```python
import functools

import jax
import jax.numpy as jnp
from jax import lax
from jax.experimental import pallas as pl
from jax.experimental.pallas import tpu as pltpu
from jax.sharding import PartitionSpec as P

epsilon = 1e-06
CORES = 2


def shards(tokens, norm_gain, routes, gate_weights, w_gate, w_up, w_down, out_gain):
    tok_rows = tokens.shape[0]
    width_local = tokens.shape[1]
    full_width = width_local * lax.axis_size("tp")
    experts = lax.axis_size("ep")
    top_count = routes.shape[1]
    capacity = 2 * top_count * tok_rows // experts
    flat_ids = routes.reshape(-1)
    onehot = (flat_ids[:, None] == jnp.arange(experts, dtype=jnp.int32)[None, :]).astype(jnp.int32)
    before = jnp.cumsum(onehot, axis=0) - onehot
    slot_index = jnp.sum(before * onehot, axis=1)
    dest_index = flat_ids * capacity + slot_index
    dest_pairs = dest_index.reshape(tok_rows, top_count)
    places = jnp.arange(experts * capacity, dtype=jnp.int32)
    scatter_mat = jnp.any(dest_pairs[None, :, :] == places[:, None, None], axis=2).astype(
        jnp.bfloat16
    )
    gate_mat = w_gate[0]
    up_mat = w_up[0]
    x_float = tokens.astype(jnp.float32)
    row_sums = lax.psum(jnp.sum(x_float * x_float, axis=1), "tp")
    scale_in = lax.rsqrt(row_sums / full_width + epsilon)
    normed = (x_float * scale_in[:, None] * norm_gain.astype(jnp.float32)).astype(jnp.bfloat16)
    outgoing = jnp.dot(scatter_mat, normed, preferred_element_type=jnp.float32).astype(jnp.bfloat16)
    arrived = lax.all_to_all(outgoing, "ep", split_axis=0, concat_axis=0, tiled=True)
    portion = lax.all_gather(arrived, "tp", axis=1, tiled=True)
    gate_sum = jnp.dot(portion, gate_mat, preferred_element_type=jnp.float32)
    up_sum = jnp.dot(portion, up_mat, preferred_element_type=jnp.float32)
    hidden = (jax.nn.silu(gate_sum) * up_sum).astype(jnp.bfloat16)
    down_mat = w_down[0]
    summed = lax.psum_scatter(
        lax.dot_general(
            down_mat, hidden, (((0,), (1,)), ((), ())), preferred_element_type=jnp.float32
        ).astype(jnp.bfloat16),
        "tp",
        scatter_dimension=0,
        tiled=True,
    )
    came_back = lax.all_to_all(summed, "ep", split_axis=1, concat_axis=1, tiled=True)
    picked = (
        jnp.take(came_back, dest_index, axis=1)
        .astype(jnp.float32)
        .reshape(width_local, tok_rows, top_count)
    )
    combined = jnp.sum(picked * gate_weights[None, :, :], axis=2).T
    out_sums = lax.psum(jnp.sum(combined * combined, axis=1), "tp")
    scale_out = lax.rsqrt(out_sums / full_width + epsilon)
    return (combined * scale_out[:, None] * out_gain.astype(jnp.float32)).astype(jnp.bfloat16)


def xor(index, mask):
    result = index
    bit = 1
    while bit <= mask:
        if mask & bit:
            result = result + bit * (1 - 2 * ((index // bit) % 2))
        bit *= 2
    return result


def plan(groups, tiles):
    steps = []

    def add(name, *args):
        steps.append((name, args))

    add("forward", 1)
    add("pass_on", 0)
    add("forward", 2)
    add("forward", 3)
    add("pass_on", 1)
    add("gain_wait")
    add("normalise", 0)
    add("pass_on", 2)
    add("normalise", 1)
    add("weight_wait", 0, 1)
    add("units", 0, 0, 2)
    add("forward", 4)
    add("pass_on", 3)
    add("units", 0, 2, 4)
    add("weight_wait", 2)
    for k in range(4):
        add("down", 0, k)
    add("normalise", 2)
    add("normalise", 3)
    add("forward", 5)
    add("across", 0)
    add("across", 1)
    add("units", 1, 0, 2)
    add("pass_on", 4)
    add("units", 1, 2, 4)
    for k in range(4):
        add("down", 1, k)
    add("pass_on", 5)
    add("forward", 6)
    add("back", 0)
    add("back", 1)
    add("normalise", 4)
    add("normalise", 5)
    add("across", 2)
    add("across", 3)
    add("units", 2, 0, 2)
    add("pass_on", 6)
    add("forward", 7)
    add("units", 2, 2, 4)
    for k in range(4):
        add("down", 2, k)
    add("across", 4)
    add("across", 5)
    add("back", 2)
    add("back", 3)
    add("normalise", 6)
    add("pass_on", 7)
    add("normalise", 7)
    add("units", 3, 0, 2)
    add("back", 4)
    add("units", 3, 2, 4)
    add("back", 5)
    for k in range(4):
        add("down", 3, k)
    add("across", 6)
    add("across", 7)
    add("gather", 0, 4)
    add("back", 6)
    add("back", 7)
    add("gather", 4, 8)
    return steps


def layer(
    n_ep, cap, groups,
    routes_hbm, gates_hbm, tokens_hbm, in_gain_hbm, out_gain_hbm, wg_hbm, wu_hbm, wd_hbm,
    out_ref,
    routes_ref, gates_ref, tokens_ref, in_gain_ref, out_gain_ref,
    wg, wu, wd, picked, xall, gains, xn, hidden, psend, prec, own, xsend, xrec, rsend, back, sums, acc,
    i_sem, w_sem, disp_s, disp_r, part_s, part_r, opp_s, opp_r, rel_s, rel_r, gain_s, gain_r,
    pd_s, pd_r, xs_s, xs_r, ret_s, ret_r, ns_s, ns_r,
):
    f32, bf16 = jnp.float32, jnp.bfloat16
    ep, tp = lax.axis_index("ep"), lax.axis_index("tp")
    chip, core = tp // CORES, tp % CORES
    partner = chip * CORES + (1 - core)
    opposite = (1 - chip) * CORES + core
    diagonal = (1 - chip) * CORES + (1 - core)
    tok, width = tokens_ref.shape
    n_tp = gains.shape[0]
    full = width * n_tp
    ff = wg.shape[1]
    peer = [xor(ep, d) for d in range(n_ep)]

    barrier = pltpu.get_barrier_semaphore()
    for d in range(1, n_ep):
        pl.semaphore_signal(barrier, inc=1, device_id={"ep": peer[d]})
    for other in (partner, opposite, diagonal):
        pl.semaphore_signal(barrier, inc=1, device_id={"tp": other})

    inputs = [
        pltpu.make_async_copy(src, dst, i_sem.at[i])
        for i, (src, dst) in enumerate(
            (
                (routes_hbm, routes_ref),
                (tokens_hbm, tokens_ref),
                (in_gain_hbm, in_gain_ref),
                (gates_hbm, gates_ref),
                (out_gain_hbm, out_gain_ref),
            )
        )
    ]
    weights = [
        pltpu.make_async_copy(src.at[0], dst, w_sem.at[i])
        for i, (src, dst) in enumerate(((wg_hbm, wg), (wu_hbm, wu), (wd_hbm, wd)))
    ]
    for copy in inputs + weights:
        copy.start()

    def remote(src, dst, send, recv, where):
        return pltpu.make_async_remote_copy(
            src_ref=src, dst_ref=dst, send_sem=send, recv_sem=recv, device_id=where
        )

    diag = lax.broadcasted_iota(jnp.int32, (tok, tok), 0) == lax.broadcasted_iota(
        jnp.int32, (tok, tok), 1
    )

    def column(row):
        return jnp.sum(jnp.where(diag, row, 0.0), axis=1, keepdims=True)

    inputs[0].wait()
    routes = routes_ref[...].astype(f32)
    first, second = column(routes[0:1]), column(routes[1:2])
    lanes = 128 * pl.cdiv(n_ep, 128)
    lane = lax.broadcasted_iota(jnp.int32, (tok, lanes), 1)
    expert = lane.astype(f32)
    is_first, is_second = expert == first, expert == second
    member = jnp.where(is_first, 1.0, 0.0) + jnp.where(is_second, 1.0, 0.0)
    earlier = jnp.where(
        lax.broadcasted_iota(jnp.int32, (tok, tok), 1)
        < lax.broadcasted_iota(jnp.int32, (tok, tok), 0),
        1.0,
        0.0,
    )
    before = jnp.dot(earlier.astype(bf16), member.astype(bf16), preferred_element_type=f32)
    place = before + (lane ^ ep).astype(f32) * cap
    place_first = jnp.sum(jnp.where(is_first, place, 0.0), axis=1, keepdims=True)
    place_second = jnp.sum(jnp.where(is_second, place, 0.0), axis=1, keepdims=True)
    slots = lax.broadcasted_iota(jnp.int32, (tok, n_ep * cap), 1).astype(f32)
    at_first, at_second = slots == place_first, slots == place_second
    select = (jnp.where(at_first, 1.0, 0.0) + jnp.where(at_second, 1.0, 0.0)).astype(bf16)
    inputs[1].wait()
    chosen = lax.dot_general(
        select, tokens_ref[...], (((0,), (0,)), ((), ())), preferred_element_type=f32
    ).astype(bf16)
    xall[pl.ds(tp, 1), 0] = chosen[:cap][None]
    picked[...] = chosen
    inputs[2].wait()
    gains[pl.ds(tp, 1)] = in_gain_ref[...].astype(f32).reshape(1, 1, width)

    pl.semaphore_wait(barrier, n_ep - 1 + n_tp - 1)

    dispatch = {
        d: remote(
            picked.at[pl.ds(d * cap, cap)], xall.at[tp, d], disp_s.at[d], disp_r.at[d], {"ep": peer[d]}
        )
        for d in range(1, n_ep)
    }
    to_partner, to_opposite, relay = [], [], []
    for d in range(n_ep):
        block = xall.at[tp, d]
        to_partner.append(remote(block, block, part_s.at[d], part_r.at[d], {"tp": partner}))
        to_opposite.append(remote(block, block, opp_s.at[d], opp_r.at[d], {"tp": opposite}))
        far = xall.at[opposite, d]
        relay.append(remote(far, far, rel_s.at[d], rel_r.at[d], {"tp": partner}))
    gain_copies = [
        remote(gains.at[tp], gains.at[tp], gain_s.at[i], gain_r.at[i], {"tp": other})
        for i, other in enumerate((partner, opposite, diagonal))
    ]
    for d in range(1, n_ep):
        dispatch[d].start()
    to_opposite[0].start()
    to_partner[0].start()
    for copy in gain_copies:
        copy.start()

    gates = gates_ref
    group_of, where_of = {}, {}
    begin = 0
    span = []
    for g, group in enumerate(groups):
        span.append(slice(begin * cap, (begin + len(group)) * cap))
        for q, d in enumerate(group):
            group_of[d], where_of[d] = (g, q), begin + q
        begin += len(group)
    tile = min(256, ff)
    partner_copies = {
        (g, k): remote(
            psend.at[k, span[g]], prec.at[k, span[g]], pd_s.at[g, k], pd_r.at[g, k], {"tp": partner}
        )
        for g in range(len(groups))
        for k in range(2)
    }
    across = [
        remote(xsend.at[d], xrec.at[d], xs_s.at[d], xs_r.at[d], {"tp": opposite})
        for d in range(n_ep)
    ]
    returned = {
        d: remote(rsend.at[d], back.at[pl.ds(d * cap, cap)], ret_s.at[d], ret_r.at[d], {"ep": peer[d]})
        for d in range(1, n_ep)
    }

    def forward(d):
        dispatch[d].wait_recv()
        to_opposite[d].start()
        to_partner[d].start()

    def pass_on(d):
        to_opposite[d].wait_recv()
        relay[d].start()

    def gain_wait():
        for copy in gain_copies:
            copy.wait_recv()

    def weight_wait(*which):
        for i in which:
            weights[i].wait()

    def normalise(d):
        to_partner[d].wait_recv()
        relay[d].wait_recv()
        parts = [xall[j, d].astype(f32) for j in range(n_tp)]
        total = sum(jnp.sum(p * p, axis=1, keepdims=True) for p in parts)
        scale = lax.rsqrt(total / full + epsilon)
        i = where_of[d]
        for j in range(n_tp):
            xn[i * cap : (i + 1) * cap, j * width : (j + 1) * width] = (
                parts[j] * scale * gains[j]
            ).astype(bf16)

    def units(g, start, stop):
        mine = span[g]

        def body(n, carry):
            cols = pl.ds(pl.multiple_of(n * tile, tile), tile)
            gate = jnp.dot(xn[mine], wg[:, cols], preferred_element_type=f32)
            up = jnp.dot(xn[mine], wu[:, cols], preferred_element_type=f32)
            hidden[mine, cols] = (gate / (1.0 + jnp.exp(-gate)) * up).astype(bf16)
            return carry

        lax.fori_loop(start, stop, body, 0)

    targets = (diagonal, partner, opposite, tp)

    def down(g, k):
        mine = span[g]
        cols = pl.ds(pl.multiple_of(targets[k] * width, width), width)
        product = jnp.dot(hidden[mine], wd[:, cols], preferred_element_type=f32)
        if k < 2:
            psend[k, mine] = product.astype(bf16)
            partner_copies[g, k].start()
        else:
            own[k - 2, mine] = product

    def rows_of(d):
        i = where_of[d]
        return slice(i * cap, (i + 1) * cap)

    def send_across(d):
        g, q = group_of[d]
        if q == 0:
            partner_copies[g, 0].wait_recv()
        part = rows_of(d)
        xsend[d] = (own[0, part] + prec[0, part].astype(f32)).astype(bf16)
        across[d].start()

    def send_back(d):
        g, q = group_of[d]
        if q == 0:
            partner_copies[g, 1].wait_recv()
        part = rows_of(d)
        both = own[1, part] + prec[1, part].astype(f32)
        across[d].wait_recv()
        done = (both + xrec[d].astype(f32)).astype(bf16)
        if d == 0:
            back[0:cap] = done
        else:
            rsend[d] = done
            returned[d].start()

    def mixing(d0, d1):
        cols = slice(d0 * cap, d1 * cap)
        part = jnp.where(at_first[:, cols], column(gates[0:1]), 0.0) + jnp.where(
            at_second[:, cols], column(gates[1:2]), 0.0
        )
        high = part.astype(bf16)
        low = (part - high.astype(f32)).astype(bf16)
        return high, low

    def gather(d0, d1):
        if d0 == 0:
            inputs[3].wait()
        for d in range(max(d0, 1), d1):
            returned[d].wait_recv()
        high, low = mixing(d0, d1)
        rows = back[d0 * cap : d1 * cap]
        total = jnp.dot(high, rows, preferred_element_type=f32) + jnp.dot(
            low, rows, preferred_element_type=f32
        )
        if d0:
            total = total + acc[...]
        if d1 < n_ep:
            acc[...] = total
        else:
            return total

    calls = dict(
        forward=forward, pass_on=pass_on, gain_wait=gain_wait, weight_wait=weight_wait, normalise=normalise,
        units=units, down=down, across=send_across, back=send_back, gather=gather,
    )
    combined = None
    for name, args in plan(groups, ff // tile):
        combined = calls[name](*args)

    row_sum = jnp.sum(combined * combined, axis=1, keepdims=True)
    flat = jnp.sum(jnp.where(diag, row_sum, 0.0), axis=0, keepdims=True)
    sums[pl.ds(tp, 1)] = flat[None]
    norm_copies = [
        remote(sums.at[tp], sums.at[tp], ns_s.at[i], ns_r.at[i], {"tp": other})
        for i, other in enumerate((partner, opposite, diagonal))
    ]
    for copy in norm_copies:
        copy.start()

    inputs[4].wait()
    for copy in gain_copies + to_partner + to_opposite + relay + across:
        copy.wait_send()
    for copies in (dispatch, partner_copies, returned):
        for copy in copies.values():
            copy.wait_send()

    for copy in norm_copies:
        copy.wait()
    total = sum(sums[j] for j in range(n_tp))
    scale = lax.rsqrt(column(total) / full + epsilon)
    gain = out_gain_ref[...].astype(f32).reshape(1, width)
    out_ref[...] = (combined * scale * gain).astype(bf16)


def fused(tokens, norm_gain, routes, gate_weights, w_gate, w_up, w_down, out_gain):
    n_ep, n_tp = lax.axis_size("ep"), lax.axis_size("tp")
    tok, width = tokens.shape
    top_count = routes.shape[1]
    cap = 2 * top_count * tok // n_ep
    _, d_model, ff = w_gate.shape
    groups = [(d, d + 1) for d in range(0, n_ep, 2)]
    bf16, f32 = jnp.bfloat16, jnp.float32
    dma = pltpu.SemaphoreType.DMA
    vmem = pl.BlockSpec(memory_space=pltpu.VMEM)
    hbm = pl.BlockSpec(memory_space=pltpu.HBM)
    slots = n_ep * cap
    return pl.pallas_call(
        functools.partial(layer, n_ep, cap, groups),
        out_shape=jax.ShapeDtypeStruct((tok, width), bf16),
        in_specs=[hbm] * 8,
        out_specs=vmem,
        scratch_shapes=[
            pltpu.VMEM((top_count, tok), jnp.int32),
            pltpu.VMEM((top_count, tok), f32),
            pltpu.VMEM((tok, width), bf16),
            pltpu.VMEM((width,), bf16),
            pltpu.VMEM((width,), bf16),
            pltpu.VMEM((d_model, ff), bf16),
            pltpu.VMEM((d_model, ff), bf16),
            pltpu.VMEM((ff, d_model), bf16),
            pltpu.VMEM((slots, width), bf16),
            pltpu.VMEM((n_tp, n_ep, cap, width), bf16),
            pltpu.VMEM((n_tp, 1, width), f32),
            pltpu.VMEM((slots, d_model), bf16),
            pltpu.VMEM((slots, ff), bf16),
            pltpu.VMEM((2, slots, width), bf16),
            pltpu.VMEM((2, slots, width), bf16),
            pltpu.VMEM((2, slots, width), f32),
            pltpu.VMEM((n_ep, cap, width), bf16),
            pltpu.VMEM((n_ep, cap, width), bf16),
            pltpu.VMEM((n_ep, cap, width), bf16),
            pltpu.VMEM((slots, width), bf16),
            pltpu.VMEM((n_tp, 1, tok), f32),
            pltpu.VMEM((tok, width), f32),
            dma((5,)),
            dma((3,)),
            *[dma((n_ep,))] * 8,
            *[dma((3,))] * 2,
            *[dma((len(groups), 2))] * 2,
            *[dma((n_ep,))] * 4,
            *[dma((3,))] * 2,
        ],
        compiler_params=pltpu.CompilerParams(
            collective_id=0, has_side_effects=True, vmem_limit_bytes=48 * 1024 * 1024
        ),
    )(
        *[
            pltpu.with_memory_space_constraint(x, pltpu.HBM)
            for x in (routes.T, gate_weights.T, tokens, norm_gain, out_gain, w_gate, w_up, w_down)
        ]
    )


def solution(mesh):
    placed = (
        P("ep", "tp"),
        P("tp"),
        P("ep", None),
        P("ep", None),
        P("ep", None, "tp"),
        P("ep", None, "tp"),
        P("ep", "tp", None),
        P("tp"),
    )
    n_ep = mesh.shape["ep"]
    pairs = mesh.shape["tp"] == 2 * CORES and n_ep >= 8 and n_ep & (n_ep - 1) == 0
    return jax.shard_map(
        fused if pairs else shards, mesh=mesh, in_specs=placed, out_specs=P("ep", "tp"), check_vma=False
    )
```

```python
import functools

import jax
import jax.numpy as jnp
from jax import lax
from jax.experimental import pallas as pl
from jax.experimental.pallas import tpu as pltpu
from jax.sharding import PartitionSpec as P

epsilon = 1e-06
CORES = 2


def shards(tokens, norm_gain, routes, gate_weights, w_gate, w_up, w_down, out_gain):
    tok_rows = tokens.shape[0]
    width_local = tokens.shape[1]
    full_width = width_local * lax.axis_size("tp")
    experts = lax.axis_size("ep")
    top_count = routes.shape[1]
    capacity = 2 * top_count * tok_rows // experts
    flat_ids = routes.reshape(-1)
    onehot = (flat_ids[:, None] == jnp.arange(experts, dtype=jnp.int32)[None, :]).astype(jnp.int32)
    before = jnp.cumsum(onehot, axis=0) - onehot
    slot_index = jnp.sum(before * onehot, axis=1)
    dest_index = flat_ids * capacity + slot_index
    dest_pairs = dest_index.reshape(tok_rows, top_count)
    places = jnp.arange(experts * capacity, dtype=jnp.int32)
    scatter_mat = jnp.any(dest_pairs[None, :, :] == places[:, None, None], axis=2).astype(
        jnp.bfloat16
    )
    gate_mat = w_gate[0]
    up_mat = w_up[0]
    x_float = tokens.astype(jnp.float32)
    row_sums = lax.psum(jnp.sum(x_float * x_float, axis=1), "tp")
    scale_in = lax.rsqrt(row_sums / full_width + epsilon)
    normed = (x_float * scale_in[:, None] * norm_gain.astype(jnp.float32)).astype(jnp.bfloat16)
    outgoing = jnp.dot(scatter_mat, normed, preferred_element_type=jnp.float32).astype(jnp.bfloat16)
    arrived = lax.all_to_all(outgoing, "ep", split_axis=0, concat_axis=0, tiled=True)
    portion = lax.all_gather(arrived, "tp", axis=1, tiled=True)
    gate_sum = jnp.dot(portion, gate_mat, preferred_element_type=jnp.float32)
    up_sum = jnp.dot(portion, up_mat, preferred_element_type=jnp.float32)
    hidden = (jax.nn.silu(gate_sum) * up_sum).astype(jnp.bfloat16)
    down_mat = w_down[0]
    summed = lax.psum_scatter(
        lax.dot_general(
            down_mat, hidden, (((0,), (1,)), ((), ())), preferred_element_type=jnp.float32
        ).astype(jnp.bfloat16),
        "tp",
        scatter_dimension=0,
        tiled=True,
    )
    came_back = lax.all_to_all(summed, "ep", split_axis=1, concat_axis=1, tiled=True)
    picked = (
        jnp.take(came_back, dest_index, axis=1)
        .astype(jnp.float32)
        .reshape(width_local, tok_rows, top_count)
    )
    combined = jnp.sum(picked * gate_weights[None, :, :], axis=2).T
    out_sums = lax.psum(jnp.sum(combined * combined, axis=1), "tp")
    scale_out = lax.rsqrt(out_sums / full_width + epsilon)
    return (combined * scale_out[:, None] * out_gain.astype(jnp.float32)).astype(jnp.bfloat16)


def xor(index, mask):
    result = index
    bit = 1
    while bit <= mask:
        if mask & bit:
            result = result + bit * (1 - 2 * ((index // bit) % 2))
        bit *= 2
    return result


def plan():
    steps = []

    def add(name, *args):
        steps.append((name, args))

    add("forward", 1)
    add("pass_on", 0)
    add("forward", 2)
    add("pass_on", 1)
    add("gain_wait")
    add("normalise", 0)
    add("forward", 3)
    add("normalise", 1)
    add("weight_wait", 0, 1)
    add("gate", 0)
    add("up", 0)
    add("pass_on", 2)
    add("forward", 4)
    add("weight_wait", 2)
    add("down", 0, 0)
    add("down", 0, 2)
    add("down", 0, 1)
    add("pass_on", 3)
    add("across", 0)
    add("down", 0, 3)
    add("normalise", 2)
    add("normalise", 3)
    add("forward", 5)
    add("pass_on", 4)
    add("normalise", 4)
    add("gate", 1)
    add("forward", 6)
    add("up", 1)
    add("forward", 7)
    add("down", 1, 0)
    add("down", 1, 2)
    add("down", 1, 1)
    add("across", 4)
    add("pass_on", 5)
    add("down", 1, 3)
    add("across", 1)
    add("normalise", 5)
    add("gate", 2)
    add("pass_on", 6)
    add("up", 2)
    add("pass_on", 7)
    add("down", 2, 0)
    add("down", 2, 2)
    add("normalise", 6)
    add("down", 2, 1)
    add("across", 5)
    add("back", 4)
    add("normalise", 7)
    add("down", 2, 3)
    add("across", 2)
    add("gate", 3)
    add("back", 0)
    add("up", 3)
    add("down", 3, 0)
    add("down", 3, 2)
    add("back", 5)
    add("down", 3, 1)
    add("across", 6)
    add("across", 7)
    add("down", 3, 3)
    add("across", 3)
    add("back", 1)
    add("back", 2)
    add("back", 6)
    add("back", 7)
    add("back", 3)
    add("gather", 0, 6)
    add("gather", 6, 8)
    return steps


def layer(
    n_ep, cap, groups,
    routes_hbm, gates_hbm, tokens_hbm, in_gain_hbm, out_gain_hbm, wg_hbm, wu_hbm, wd_hbm,
    out_ref,
    routes_ref, gates_ref, tokens_ref, in_gain_ref, out_gain_ref,
    wg, wu, wd, picked, xall, gains, xn, hidden, psend, prec, own, xsend, xrec, rsend, back, sums, acc, gated,
    i_sem, w_sem, sent, disp_r, part_r, opp_r, gain_r, pd_r, xs_r, ret_r, ns_r,
):
    f32, bf16 = jnp.float32, jnp.bfloat16
    ep, tp = lax.axis_index("ep"), lax.axis_index("tp")
    chip, core = tp // CORES, tp % CORES
    partner = chip * CORES + (1 - core)
    opposite = (1 - chip) * CORES + core
    diagonal = (1 - chip) * CORES + (1 - core)
    tok, width = tokens_ref.shape
    n_tp = gains.shape[0]
    full = width * n_tp
    ff = wg.shape[1]
    peer = [xor(ep, d) for d in range(n_ep)]

    barrier = pltpu.get_barrier_semaphore()
    for d in range(1, n_ep):
        pl.semaphore_signal(barrier, inc=1, device_id={"ep": peer[d]})
    for other in (partner, opposite, diagonal):
        pl.semaphore_signal(barrier, inc=1, device_id={"tp": other})

    inputs = [
        pltpu.make_async_copy(src, dst, i_sem.at[i])
        for i, (src, dst) in enumerate(
            (
                (routes_hbm, routes_ref),
                (tokens_hbm, tokens_ref),
                (in_gain_hbm, in_gain_ref),
                (gates_hbm, gates_ref),
                (out_gain_hbm, out_gain_ref),
            )
        )
    ]
    weights = [
        pltpu.make_async_copy(src.at[0], dst, w_sem.at[i])
        for i, (src, dst) in enumerate(((wg_hbm, wg), (wu_hbm, wu), (wd_hbm, wd)))
    ]
    for copy in inputs + weights:
        copy.start()

    def wait_bytes(ref, sem):
        pltpu.make_async_copy(ref, ref, sem).wait()

    def remote(src, dst, send, recv, where):
        return pltpu.make_async_remote_copy(
            src_ref=src, dst_ref=dst, send_sem=send, recv_sem=recv, device_id=where
        )

    diag = lax.broadcasted_iota(jnp.int32, (tok, tok), 0) == lax.broadcasted_iota(
        jnp.int32, (tok, tok), 1
    )

    def column(row):
        return jnp.sum(jnp.where(diag, row, 0.0), axis=1, keepdims=True)

    inputs[0].wait()
    routes = routes_ref[...].astype(f32)
    first, second = column(routes[0:1]), column(routes[1:2])
    lanes = 128 * pl.cdiv(n_ep, 128)
    lane = lax.broadcasted_iota(jnp.int32, (tok, lanes), 1)
    expert = lane.astype(f32)
    is_first, is_second = expert == first, expert == second
    member = jnp.where(is_first, 1.0, 0.0) + jnp.where(is_second, 1.0, 0.0)
    earlier = jnp.where(
        lax.broadcasted_iota(jnp.int32, (tok, tok), 1)
        < lax.broadcasted_iota(jnp.int32, (tok, tok), 0),
        1.0,
        0.0,
    )
    before = jnp.dot(earlier.astype(bf16), member.astype(bf16), preferred_element_type=f32)
    place = before + (lane ^ ep).astype(f32) * cap
    place_first = jnp.sum(jnp.where(is_first, place, 0.0), axis=1, keepdims=True)
    place_second = jnp.sum(jnp.where(is_second, place, 0.0), axis=1, keepdims=True)
    slots = lax.broadcasted_iota(jnp.int32, (tok, n_ep * cap), 1).astype(f32)
    at_first, at_second = slots == place_first, slots == place_second
    select = (jnp.where(at_first, 1.0, 0.0) + jnp.where(at_second, 1.0, 0.0)).astype(bf16)
    inputs[1].wait()
    chosen = lax.dot_general(
        select, tokens_ref[...], (((0,), (0,)), ((), ())), preferred_element_type=f32
    ).astype(bf16)
    xall[pl.ds(tp, 1), 0] = chosen[:cap][None]
    picked[...] = chosen
    inputs[2].wait()
    gains[pl.ds(tp, 1)] = in_gain_ref[...].astype(f32).reshape(1, 1, width)

    pl.semaphore_wait(barrier, n_ep - 1 + n_tp - 1)

    dispatch = {
        d: remote(
            picked.at[pl.ds(d * cap, cap)], xall.at[tp, d], sent.at[0], disp_r.at[d], {"ep": peer[d]}
        )
        for d in range(1, n_ep)
    }
    to_partner, to_opposite, relay = [], [], []
    for d in range(n_ep):
        block = xall.at[tp, d]
        to_partner.append(remote(block, block, sent.at[1], part_r.at[d], {"tp": partner}))
        to_opposite.append(remote(block, block, sent.at[2], opp_r.at[d], {"tp": opposite}))
        far = xall.at[opposite, d]
        relay.append(remote(far, far, sent.at[3], part_r.at[d], {"tp": partner}))
    gain_copies = [
        remote(gains.at[tp], gains.at[tp], sent.at[4], gain_r.at[0], {"tp": other})
        for i, other in enumerate((partner, opposite, diagonal))
    ]
    to_opposite[0].start()
    to_partner[0].start()
    for d in (1,2,3,4,5,6,7):
        dispatch[d].start()
    for copy in gain_copies:
        copy.start()

    gates = gates_ref
    part_of = {d: 0 if d < 6 else 1 for d in range(n_ep)}
    group_of, where_of = {}, {}
    begin = 0
    span = []
    for g, group in enumerate(groups):
        span.append(slice(begin * cap, (begin + len(group)) * cap))
        for q, d in enumerate(group):
            group_of[d], where_of[d] = g, begin + q
        begin += len(group)
    partner_copies = {
        (g, k): remote(
            psend.at[k, span[g]], prec.at[k, span[g]], sent.at[5], pd_r.at[g, k], {"tp": partner}
        )
        for g in range(len(groups))
        for k in range(2)
    }
    across = [
        remote(xsend.at[d], xrec.at[d], sent.at[6], xs_r.at[d], {"tp": opposite})
        for d in range(n_ep)
    ]
    returned = {
        d: remote(rsend.at[d], back.at[pl.ds(d * cap, cap)], sent.at[7], ret_r.at[part_of[d]], {"ep": peer[d]})
        for d in range(1, n_ep)
    }

    def forward(d):
        dispatch[d].wait_recv()
        to_opposite[d].start()
        to_partner[d].start()

    def pass_on(d):
        to_opposite[d].wait_recv()
        relay[d].start()

    def gain_wait():
        wait_bytes(gains.at[pl.ds(0, n_tp - 1)], gain_r.at[0])

    def weight_wait(*which):
        for i in which:
            weights[i].wait()

    def normalise(d):
        wait_bytes(xall.at[pl.ds(0, CORES), d], part_r.at[d])
        parts = [xall[j, d].astype(f32) for j in range(n_tp)]
        total = sum(jnp.sum(p * p, axis=1, keepdims=True) for p in parts)
        scale = lax.rsqrt(total / full + epsilon)
        i = where_of[d]
        for j in range(n_tp):
            xn[i * cap : (i + 1) * cap, j * width : (j + 1) * width] = (
                parts[j] * scale * gains[j]
            ).astype(bf16)

    def gate(g):
        gated[: cap * len(groups[g])] = jnp.dot(xn[span[g]], wg[...], preferred_element_type=f32)

    def up(g):
        value = gated[: cap * len(groups[g])]
        product = jnp.dot(xn[span[g]], wu[...], preferred_element_type=f32)
        hidden[span[g]] = (value / (1.0 + jnp.exp(-value)) * product).astype(bf16)

    targets = (diagonal, partner, opposite, tp)

    def down(g, k):
        mine = span[g]
        cols = pl.ds(pl.multiple_of(targets[k] * width, width), width)
        product = jnp.dot(hidden[mine], wd[:, cols], preferred_element_type=f32)
        if k < 2:
            psend[k, mine] = product.astype(bf16)
            partner_copies[g, k].start()
        else:
            own[k - 2, mine] = product

    waited = set()

    def have(g, k):
        if (g, k) not in waited:
            waited.add((g, k))
            partner_copies[g, k].wait_recv()

    def rows_of(d):
        i = where_of[d]
        return slice(i * cap, (i + 1) * cap)

    def send_across(d):
        have(group_of[d], 0)
        part = rows_of(d)
        xsend[d] = (own[0, part] + prec[0, part].astype(f32)).astype(bf16)
        across[d].start()

    def send_back(d):
        have(group_of[d], 1)
        part = rows_of(d)
        both = own[1, part] + prec[1, part].astype(f32)
        across[d].wait_recv()
        done = (both + xrec[d].astype(f32)).astype(bf16)
        if d == 0:
            back[0:cap] = done
        else:
            rsend[d] = done
            returned[d].start()

    def mixing(d0, d1):
        cols = slice(d0 * cap, d1 * cap)
        part = jnp.where(at_first[:, cols], column(gates[0:1]), 0.0) + jnp.where(
            at_second[:, cols], column(gates[1:2]), 0.0
        )
        high = part.astype(bf16)
        low = (part - high.astype(f32)).astype(bf16)
        return high, low

    def gather(d0, d1):
        if d0 == 0:
            inputs[3].wait()
        lo = max(d0, 1)
        wait_bytes(back.at[pl.ds(lo * cap, (d1 - lo) * cap)], ret_r.at[part_of[lo]])
        high, low = mixing(d0, d1)
        rows = back[d0 * cap : d1 * cap]
        total = jnp.dot(high, rows, preferred_element_type=f32) + jnp.dot(
            low, rows, preferred_element_type=f32
        )
        if d0:
            total = total + acc[...]
        if d1 < n_ep:
            acc[...] = total
        else:
            return total

    calls = dict(
        forward=forward, pass_on=pass_on, gain_wait=gain_wait, weight_wait=weight_wait, normalise=normalise,
        gate=gate, up=up, down=down, across=send_across, back=send_back, gather=gather,
    )
    combined = None
    for name, args in plan():
        combined = calls[name](*args)

    row_sum = jnp.sum(combined * combined, axis=1, keepdims=True)
    flat = jnp.sum(jnp.where(diag, row_sum, 0.0), axis=0, keepdims=True)
    sums[pl.ds(tp, 1)] = flat[None]
    norm_copies = [
        remote(sums.at[tp], sums.at[tp], sent.at[8], ns_r.at[0], {"tp": other})
        for i, other in enumerate((partner, opposite, diagonal))
    ]
    for copy in norm_copies:
        copy.start()

    inputs[4].wait()
    blocks = xall.at[0]
    wait_bytes(picked.at[pl.ds(0, (n_ep - 1) * cap)], sent.at[0])
    for i in (1, 2, 3):
        wait_bytes(blocks, sent.at[i])
    wait_bytes(gains.at[pl.ds(0, n_tp - 1)], sent.at[4])
    wait_bytes(psend, sent.at[5])
    wait_bytes(xsend, sent.at[6])
    wait_bytes(rsend.at[pl.ds(0, n_ep - 1)], sent.at[7])

    wait_bytes(sums.at[pl.ds(0, n_tp - 1)], ns_r.at[0])
    wait_bytes(sums.at[pl.ds(0, n_tp - 1)], sent.at[8])
    total = sum(sums[j] for j in range(n_tp))
    scale = lax.rsqrt(column(total) / full + epsilon)
    gain = out_gain_ref[...].astype(f32).reshape(1, width)
    out_ref[...] = (combined * scale * gain).astype(bf16)


def fused(tokens, norm_gain, routes, gate_weights, w_gate, w_up, w_down, out_gain):
    n_ep, n_tp = lax.axis_size("ep"), lax.axis_size("tp")
    tok, width = tokens.shape
    top_count = routes.shape[1]
    cap = 2 * top_count * tok // n_ep
    _, d_model, ff = w_gate.shape
    groups = [(0,1),(2,4),(3,5),(6,7)]
    bf16, f32 = jnp.bfloat16, jnp.float32
    dma = pltpu.SemaphoreType.DMA
    vmem = pl.BlockSpec(memory_space=pltpu.VMEM)
    hbm = pl.BlockSpec(memory_space=pltpu.HBM)
    slots = n_ep * cap
    return pl.pallas_call(
        functools.partial(layer, n_ep, cap, groups),
        out_shape=jax.ShapeDtypeStruct((tok, width), bf16),
        in_specs=[hbm] * 8,
        out_specs=vmem,
        scratch_shapes=[
            pltpu.VMEM((top_count, tok), jnp.int32),
            pltpu.VMEM((top_count, tok), f32),
            pltpu.VMEM((tok, width), bf16),
            pltpu.VMEM((width,), bf16),
            pltpu.VMEM((width,), bf16),
            pltpu.VMEM((d_model, ff), bf16),
            pltpu.VMEM((d_model, ff), bf16),
            pltpu.VMEM((ff, d_model), bf16),
            pltpu.VMEM((slots, width), bf16),
            pltpu.VMEM((n_tp, n_ep, cap, width), bf16),
            pltpu.VMEM((n_tp, 1, width), f32),
            pltpu.VMEM((slots, d_model), bf16),
            pltpu.VMEM((slots, ff), bf16),
            pltpu.VMEM((2, slots, width), bf16),
            pltpu.VMEM((2, slots, width), bf16),
            pltpu.VMEM((2, slots, width), f32),
            pltpu.VMEM((n_ep, cap, width), bf16),
            pltpu.VMEM((n_ep, cap, width), bf16),
            pltpu.VMEM((n_ep, cap, width), bf16),
            pltpu.VMEM((slots, width), bf16),
            pltpu.VMEM((n_tp, 1, tok), f32),
            pltpu.VMEM((tok, width), f32),
            pltpu.VMEM((max(map(len, groups)) * cap, ff), f32),
            dma((5,)),
            dma((3,)),
            dma((9,)),
            *[dma((n_ep,))] * 3,
            dma((1,)),
            dma((len(groups), 2)),
            dma((n_ep,)),
            dma((2,)),
            dma((1,)),
        ],
        compiler_params=pltpu.CompilerParams(
            collective_id=0, has_side_effects=True, vmem_limit_bytes=48 * 1024 * 1024
        ),
    )(
        *[
            pltpu.with_memory_space_constraint(x, pltpu.HBM)
            for x in (routes.T, gate_weights.T, tokens, norm_gain, out_gain, w_gate, w_up, w_down)
        ]
    )


def solution(mesh):
    placed = (
        P("ep", "tp"),
        P("tp"),
        P("ep", None),
        P("ep", None),
        P("ep", None, "tp"),
        P("ep", None, "tp"),
        P("ep", "tp", None),
        P("tp"),
    )
    n_ep = mesh.shape["ep"]
    pairs = mesh.shape["tp"] == 2 * CORES and n_ep >= 8 and n_ep & (n_ep - 1) == 0
    return jax.shard_map(
        fused if pairs else shards, mesh=mesh, in_specs=placed, out_specs=P("ep", "tp"), check_vma=False
    )
```

```python
import functools

import jax
import jax.numpy as jnp
from jax import lax
from jax.experimental import pallas as pl
from jax.experimental.pallas import tpu as pltpu
from jax.sharding import PartitionSpec as P

epsilon = 1e-06
CORES = 2
GROUPS = ((0, 1), (2, 4), (3, 5), (6, 7))


def shards(tokens, norm_gain, routes, gate_weights, w_gate, w_up, w_down, out_gain):
    tok_rows = tokens.shape[0]
    width_local = tokens.shape[1]
    full_width = width_local * lax.axis_size("tp")
    experts = lax.axis_size("ep")
    top_count = routes.shape[1]
    capacity = 2 * top_count * tok_rows // experts
    flat_ids = routes.reshape(-1)
    onehot = (flat_ids[:, None] == jnp.arange(experts, dtype=jnp.int32)[None, :]).astype(jnp.int32)
    before = jnp.cumsum(onehot, axis=0) - onehot
    slot_index = jnp.sum(before * onehot, axis=1)
    dest_index = flat_ids * capacity + slot_index
    dest_pairs = dest_index.reshape(tok_rows, top_count)
    places = jnp.arange(experts * capacity, dtype=jnp.int32)
    scatter_mat = jnp.any(dest_pairs[None, :, :] == places[:, None, None], axis=2).astype(
        jnp.bfloat16
    )
    gate_mat = w_gate[0]
    up_mat = w_up[0]
    x_float = tokens.astype(jnp.float32)
    row_sums = lax.psum(jnp.sum(x_float * x_float, axis=1), "tp")
    scale_in = lax.rsqrt(row_sums / full_width + epsilon)
    normed = (x_float * scale_in[:, None] * norm_gain.astype(jnp.float32)).astype(jnp.bfloat16)
    outgoing = jnp.dot(scatter_mat, normed, preferred_element_type=jnp.float32).astype(jnp.bfloat16)
    arrived = lax.all_to_all(outgoing, "ep", split_axis=0, concat_axis=0, tiled=True)
    portion = lax.all_gather(arrived, "tp", axis=1, tiled=True)
    gate_sum = jnp.dot(portion, gate_mat, preferred_element_type=jnp.float32)
    up_sum = jnp.dot(portion, up_mat, preferred_element_type=jnp.float32)
    hidden = (jax.nn.silu(gate_sum) * up_sum).astype(jnp.bfloat16)
    down_mat = w_down[0]
    summed = lax.psum_scatter(
        lax.dot_general(
            down_mat, hidden, (((0,), (1,)), ((), ())), preferred_element_type=jnp.float32
        ).astype(jnp.bfloat16),
        "tp",
        scatter_dimension=0,
        tiled=True,
    )
    came_back = lax.all_to_all(summed, "ep", split_axis=1, concat_axis=1, tiled=True)
    picked = (
        jnp.take(came_back, dest_index, axis=1)
        .astype(jnp.float32)
        .reshape(width_local, tok_rows, top_count)
    )
    combined = jnp.sum(picked * gate_weights[None, :, :], axis=2).T
    out_sums = lax.psum(jnp.sum(combined * combined, axis=1), "tp")
    scale_out = lax.rsqrt(out_sums / full_width + epsilon)
    return (combined * scale_out[:, None] * out_gain.astype(jnp.float32)).astype(jnp.bfloat16)


def xor(index, mask):
    result = index
    bit = 1
    while bit <= mask:
        if mask & bit:
            result = result + bit * (1 - 2 * ((index // bit) % 2))
        bit *= 2
    return result


def plan():
    steps = []

    def add(name, *args):
        steps.append((name, args))

    add("forward", 1)
    add("gain_wait")
    add("pass_on", 1)
    add("pass_on", 0)
    add("forward", 2)
    add("normalise", 1)
    add("forward", 4)
    add("weight_wait", 0, 1)
    add("normalise", 0)
    add("gate", 0)
    add("weight_wait", 2)
    add("pass_on", 2)
    add("forward", 3)
    add("up", 0)
    add("forward", 6)
    add("pass_on", 4)
    add("normalise", 2)
    add("down", 0, 0)
    add("forward", 5)
    add("normalise", 4)
    add("gate", 1)
    add("up", 1)
    add("pass_on", 3)
    add("forward", 7)
    add("down", 1, 0)
    add("down", 0, 1)
    add("down", 1, 2)
    add("down", 1, 1)
    add("down", 0, 2)
    add("across", 4)
    add("pass_on", 5)
    add("across", 1)
    add("normalise", 3)
    add("down", 1, 3)
    add("down", 0, 3)
    add("normalise", 5)
    add("gate", 2)
    add("pass_on", 6)
    add("across", 0)
    add("up", 2)
    add("pass_on", 7)
    add("down", 2, 0)
    add("down", 2, 2)
    add("normalise", 6)
    add("down", 2, 1)
    add("across", 5)
    add("back", 4)
    add("normalise", 7)
    add("gate", 3)
    add("across", 2)
    add("up", 3)
    add("down", 3, 0)
    add("down", 3, 2)
    add("down", 2, 3)
    add("back", 1)
    add("across", 7)
    add("down", 3, 1)
    add("across", 6)
    add("across", 3)
    add("back", 5)
    add("back", 2)
    add("down", 3, 3)
    add("back", 7)
    add("back", 6)
    add("back", 3)
    add("back", 0)
    add("gather", 0, 6)
    add("gather", 6, 8)
    return steps


def layer(
    n_ep, cap, groups,
    routes_hbm, gates_hbm, tokens_hbm, in_gain_hbm, out_gain_hbm, wg_hbm, wu_hbm, wd_hbm,
    out_ref,
    routes_ref, gates_ref, tokens_ref, in_gain_ref, out_gain_ref,
    wg, wu, wd, picked, xall, gains, xn, hidden, psend, prec, own, xsend, xrec, rsend, back, sums, acc, gated,
    i_sem, w_sem, sent, disp_r, part_r, opp_r, gain_r, pd_r, xs_r, ret_r, ns_r,
):
    f32, bf16 = jnp.float32, jnp.bfloat16
    ep, tp = lax.axis_index("ep"), lax.axis_index("tp")
    chip, core = tp // CORES, tp % CORES
    partner = chip * CORES + (1 - core)
    opposite = (1 - chip) * CORES + core
    diagonal = (1 - chip) * CORES + (1 - core)
    tok, width = tokens_ref.shape
    n_tp = gains.shape[0]
    full = width * n_tp
    ff = wg.shape[1]
    peer = [xor(ep, d) for d in range(n_ep)]

    barrier = pltpu.get_barrier_semaphore()
    for d in range(1, n_ep):
        pl.semaphore_signal(barrier, inc=1, device_id={"ep": peer[d]})
    for other in (partner, opposite, diagonal):
        pl.semaphore_signal(barrier, inc=1, device_id={"tp": other})

    inputs = [
        pltpu.make_async_copy(src, dst, i_sem.at[i])
        for i, (src, dst) in enumerate(
            (
                (routes_hbm, routes_ref),
                (tokens_hbm, tokens_ref),
                (in_gain_hbm, in_gain_ref),
                (gates_hbm, gates_ref),
                (out_gain_hbm, out_gain_ref),
            )
        )
    ]
    weights = [
        pltpu.make_async_copy(src.at[0], dst, w_sem.at[i])
        for i, (src, dst) in enumerate(((wg_hbm, wg), (wu_hbm, wu), (wd_hbm, wd)))
    ]
    for copy in inputs + weights:
        copy.start()

    def wait_bytes(ref, sem):
        pltpu.make_async_copy(ref, ref, sem).wait()

    def remote(src, dst, send, recv, where):
        return pltpu.make_async_remote_copy(
            src_ref=src, dst_ref=dst, send_sem=send, recv_sem=recv, device_id=where
        )

    diag = lax.broadcasted_iota(jnp.int32, (tok, tok), 0) == lax.broadcasted_iota(
        jnp.int32, (tok, tok), 1
    )

    def column(row):
        return jnp.sum(jnp.where(diag, row, 0.0), axis=1, keepdims=True)

    def places(shape, tokens_at, first, second, count):
        one = lax.broadcasted_iota(jnp.int32, shape, 1 - tokens_at)
        expert = one.astype(f32)
        is_first, is_second = expert == first, expert == second
        member = jnp.where(is_first, 1.0, 0.0) + jnp.where(is_second, 1.0, 0.0)
        place = count(member.astype(bf16)) + (one ^ ep).astype(f32) * cap
        return tuple(
            jnp.sum(jnp.where(chosen_one, place, 0.0), axis=1 - tokens_at, keepdims=True)
            for chosen_one in (is_first, is_second)
        )

    later = jnp.where(
        lax.broadcasted_iota(jnp.int32, (tok, tok), 0)
        < lax.broadcasted_iota(jnp.int32, (tok, tok), 1),
        1.0,
        0.0,
    ).astype(bf16)
    slots = lax.broadcasted_iota(jnp.int32, (n_ep * cap, tok), 0).astype(f32)
    inputs[0].wait()
    routes = routes_ref[...].astype(f32)
    row_first, row_second = places(
        (n_ep, tok), 1, routes[0:1], routes[1:2],
        lambda member: jnp.dot(member, later, preferred_element_type=f32),
    )
    select = (
        jnp.where(slots == row_first, 1.0, 0.0) + jnp.where(slots == row_second, 1.0, 0.0)
    ).astype(bf16)
    inputs[1].wait()
    chosen = jnp.dot(select, tokens_ref[...], preferred_element_type=f32).astype(bf16)
    xall[pl.ds(tp, 1), 0] = chosen[:cap][None]
    picked[...] = chosen
    inputs[2].wait()
    gains[pl.ds(tp, 1)] = in_gain_ref[...].astype(f32).reshape(1, 1, width)

    pl.semaphore_wait(barrier, n_ep - 1 + n_tp - 1)

    dispatch = {
        d: remote(
            picked.at[pl.ds(d * cap, cap)], xall.at[tp, d], sent.at[0], disp_r.at[d], {"ep": peer[d]}
        )
        for d in range(1, n_ep)
    }
    to_partner, to_opposite, relay = [], [], []
    for d in range(n_ep):
        block = xall.at[tp, d]
        to_partner.append(remote(block, block, sent.at[1], part_r.at[d], {"tp": partner}))
        to_opposite.append(remote(block, block, sent.at[2], opp_r.at[d], {"tp": opposite}))
        far = xall.at[opposite, d]
        relay.append(remote(far, far, sent.at[3], part_r.at[d], {"tp": partner}))
    gain_copies = [
        remote(gains.at[tp], gains.at[tp], sent.at[4], gain_r.at[0], {"tp": other})
        for i, other in enumerate((partner, opposite, diagonal))
    ]
    to_opposite[0].start()
    to_partner[0].start()
    for d in (1,2,3,4,5,6,7):
        dispatch[d].start()
    for copy in gain_copies:
        copy.start()

    gates = gates_ref
    part_of = {d: 0 if d < 6 else 1 for d in range(n_ep)}
    group_of, where_of = {}, {}
    begin = 0
    span = []
    for g, group in enumerate(groups):
        span.append(slice(begin * cap, (begin + len(group)) * cap))
        for q, d in enumerate(group):
            group_of[d], where_of[d] = g, begin + q
        begin += len(group)
    partner_copies = {
        (g, k): remote(
            psend.at[k, span[g]], prec.at[k, span[g]], sent.at[5], pd_r.at[g, k], {"tp": partner}
        )
        for g in range(len(groups))
        for k in range(2)
    }
    across = [
        remote(xsend.at[d], xrec.at[d], sent.at[6], xs_r.at[d], {"tp": opposite})
        for d in range(n_ep)
    ]
    returned = {
        d: remote(rsend.at[d], back.at[pl.ds(d * cap, cap)], sent.at[7], ret_r.at[part_of[d]], {"ep": peer[d]})
        for d in range(1, n_ep)
    }

    def forward(d):
        dispatch[d].wait_recv()
        to_opposite[d].start()
        to_partner[d].start()

    def pass_on(d):
        to_opposite[d].wait_recv()
        relay[d].start()

    def gain_wait():
        wait_bytes(gains.at[pl.ds(0, n_tp - 1)], gain_r.at[0])

    def weight_wait(*which):
        for i in which:
            weights[i].wait()

    def normalise(d):
        wait_bytes(xall.at[pl.ds(0, CORES), d], part_r.at[d])
        parts = [xall[j, d].astype(f32) for j in range(n_tp)]
        total = sum(jnp.sum(p * p, axis=1, keepdims=True) for p in parts)
        scale = lax.rsqrt(total / full + epsilon)
        i = where_of[d]
        for j in range(n_tp):
            xn[i * cap : (i + 1) * cap, j * width : (j + 1) * width] = (
                parts[j] * scale * gains[j]
            ).astype(bf16)

    def gate(g):
        gated[: cap * len(groups[g])] = jnp.dot(xn[span[g]], wg[...], preferred_element_type=f32)

    def up(g):
        value = gated[: cap * len(groups[g])]
        product = jnp.dot(xn[span[g]], wu[...], preferred_element_type=f32)
        hidden[span[g]] = (value / (1.0 + jnp.exp(-value)) * product).astype(bf16)

    targets = (diagonal, partner, opposite, tp)

    def down(g, k):
        mine = span[g]
        cols = pl.ds(pl.multiple_of(targets[k] * width, width), width)
        product = jnp.dot(hidden[mine], wd[:, cols], preferred_element_type=f32)
        if k < 2:
            psend[k, mine] = product.astype(bf16)
            partner_copies[g, k].start()
        else:
            own[k - 2, mine] = product

    waited = set()

    def have(g, k):
        if (g, k) not in waited:
            waited.add((g, k))
            partner_copies[g, k].wait_recv()

    def rows_of(d):
        i = where_of[d]
        return slice(i * cap, (i + 1) * cap)

    def send_across(d):
        have(group_of[d], 0)
        part = rows_of(d)
        xsend[d] = (own[0, part] + prec[0, part].astype(f32)).astype(bf16)
        across[d].start()

    def send_back(d):
        have(group_of[d], 1)
        part = rows_of(d)
        both = own[1, part] + prec[1, part].astype(f32)
        across[d].wait_recv()
        done = (both + xrec[d].astype(f32)).astype(bf16)
        if d == 0:
            back[0:cap] = done
        else:
            rsend[d] = done
            returned[d].start()

    def mixing(d0, d1):
        slot = lax.broadcasted_iota(jnp.int32, (tok, (d1 - d0) * cap), 1).astype(f32) + d0 * cap
        part = jnp.where(slot == column(row_first), column(gates[0:1]), 0.0) + jnp.where(
            slot == column(row_second), column(gates[1:2]), 0.0
        )
        high = part.astype(bf16)
        low = (part - high.astype(f32)).astype(bf16)
        return high, low

    def gather(d0, d1):
        if d0 == 0:
            inputs[3].wait()
        high, low = mixing(d0, d1)
        lo = max(d0, 1)
        wait_bytes(back.at[pl.ds(lo * cap, (d1 - lo) * cap)], ret_r.at[part_of[lo]])
        rows = back[d0 * cap : d1 * cap]
        total = jnp.dot(high, rows, preferred_element_type=f32) + jnp.dot(
            low, rows, preferred_element_type=f32
        )
        if d0:
            total = total + acc[...]
        if d1 < n_ep:
            acc[...] = total
        else:
            return total

    calls = dict(
        forward=forward, pass_on=pass_on, gain_wait=gain_wait, weight_wait=weight_wait, normalise=normalise,
        gate=gate, up=up, down=down, across=send_across, back=send_back, gather=gather,
    )
    combined = None
    for name, args in plan():
        combined = calls[name](*args)

    row_sum = jnp.sum(combined * combined, axis=1, keepdims=True)
    flat = jnp.sum(jnp.where(diag, row_sum, 0.0), axis=0, keepdims=True)
    sums[pl.ds(tp, 1)] = flat[None]
    norm_copies = [
        remote(sums.at[tp], sums.at[tp], sent.at[8], ns_r.at[0], {"tp": other})
        for i, other in enumerate((partner, opposite, diagonal))
    ]
    for copy in norm_copies:
        copy.start()

    inputs[4].wait()
    blocks = xall.at[0]
    wait_bytes(picked.at[pl.ds(0, (n_ep - 1) * cap)], sent.at[0])
    for i in (1, 2, 3):
        wait_bytes(blocks, sent.at[i])
    wait_bytes(gains.at[pl.ds(0, n_tp - 1)], sent.at[4])
    wait_bytes(psend, sent.at[5])
    wait_bytes(xsend, sent.at[6])
    wait_bytes(rsend.at[pl.ds(0, n_ep - 1)], sent.at[7])

    wait_bytes(sums.at[pl.ds(0, n_tp - 1)], ns_r.at[0])
    wait_bytes(sums.at[pl.ds(0, n_tp - 1)], sent.at[8])
    total = sum(sums[j] for j in range(n_tp))
    scale = lax.rsqrt(column(total) / full + epsilon)
    gain = out_gain_ref[...].astype(f32).reshape(1, width)
    out_ref[...] = (combined * scale * gain).astype(bf16)


def fused(tokens, norm_gain, routes, gate_weights, w_gate, w_up, w_down, out_gain):
    n_ep, n_tp = lax.axis_size("ep"), lax.axis_size("tp")
    tok, width = tokens.shape
    top_count = routes.shape[1]
    cap = 2 * top_count * tok // n_ep
    _, d_model, ff = w_gate.shape
    groups = GROUPS
    bf16, f32 = jnp.bfloat16, jnp.float32
    dma = pltpu.SemaphoreType.DMA
    vmem = pl.BlockSpec(memory_space=pltpu.VMEM)
    hbm = pl.BlockSpec(memory_space=pltpu.HBM)
    slots = n_ep * cap
    return pl.pallas_call(
        functools.partial(layer, n_ep, cap, groups),
        out_shape=jax.ShapeDtypeStruct((tok, width), bf16),
        in_specs=[hbm] * 8,
        out_specs=vmem,
        scratch_shapes=[
            pltpu.VMEM((top_count, tok), jnp.int32),
            pltpu.VMEM((top_count, tok), f32),
            pltpu.VMEM((tok, width), bf16),
            pltpu.VMEM((width,), bf16),
            pltpu.VMEM((width,), bf16),
            pltpu.VMEM((d_model, ff), bf16),
            pltpu.VMEM((d_model, ff), bf16),
            pltpu.VMEM((ff, d_model), bf16),
            pltpu.VMEM((slots, width), bf16),
            pltpu.VMEM((n_tp, n_ep, cap, width), bf16),
            pltpu.VMEM((n_tp, 1, width), f32),
            pltpu.VMEM((slots, d_model), bf16),
            pltpu.VMEM((slots, ff), bf16),
            pltpu.VMEM((2, slots, width), bf16),
            pltpu.VMEM((2, slots, width), bf16),
            pltpu.VMEM((2, slots, width), f32),
            pltpu.VMEM((n_ep, cap, width), bf16),
            pltpu.VMEM((n_ep, cap, width), bf16),
            pltpu.VMEM((n_ep, cap, width), bf16),
            pltpu.VMEM((slots, width), bf16),
            pltpu.VMEM((n_tp, 1, tok), f32),
            pltpu.VMEM((tok, width), f32),
            pltpu.VMEM((max(map(len, groups)) * cap, ff), f32),
            dma((5,)),
            dma((3,)),
            dma((9,)),
            *[dma((n_ep,))] * 3,
            dma((1,)),
            dma((len(groups), 2)),
            dma((n_ep,)),
            dma((2,)),
            dma((1,)),
        ],
        compiler_params=pltpu.CompilerParams(
            collective_id=0, has_side_effects=True, vmem_limit_bytes=48 * 1024 * 1024
        ),
    )(
        *[
            pltpu.with_memory_space_constraint(x, pltpu.HBM)
            for x in (routes.T, gate_weights.T, tokens, norm_gain, out_gain, w_gate, w_up, w_down)
        ]
    )


def solution(mesh):
    placed = (
        P("ep", "tp"),
        P("tp"),
        P("ep", None),
        P("ep", None),
        P("ep", None, "tp"),
        P("ep", None, "tp"),
        P("ep", "tp", None),
        P("tp"),
    )
    n_ep = mesh.shape["ep"]
    pairs = mesh.shape["tp"] == 2 * CORES and n_ep == sum(map(len, GROUPS))
    return jax.shard_map(
        fused if pairs else shards, mesh=mesh, in_specs=placed, out_specs=P("ep", "tp"), check_vma=False
    )
```
